32 devices in a mesh: row: 8 (over z, core), col: 4 (over y, x).
Axes of the slice: x: 2, y: 2, z: 4, core: 2. Of those that a mesh axis runs over, the one named last changes fastest.
Arguments:
- mix_input: bfloat16 [4, 2048, 1024], P('col', 'row'), may hold values from -6 to 6
- gate_logits: bfloat16 [4, 2048, 2048], P('col', 'row'), may hold values from -8 to 8
- w_proj: bfloat16 [1024, 2048], P('col'), may hold values from -0.1875 to 0.1875
Outputs:
- mixed: bfloat16 [4, 2048, 2048], P('col', 'row')
The draws below stay inside these ranges and needn't reach their ends.
All inputs are finite; a program needn't handle non-finite values.
Results may differ from the reference program's by a relative error of at most 0.0049.
Values may be sent and summed in bfloat16 or wider, within the bound.
A program may use at most 64 MiB of HBM per device.

```python
import jax
import jax.numpy as jnp
from jax import lax

D = 2048
GROUP = 256
GROUPS = 4
F = 1024
LENGTH = 2048
SEQS = 4


def steps_of(rng, dims, shards, smallest, top_value):
    factor_of = 1.0
    for axis_at, blocks in shards:
        steps = jax.random.uniform(jax.random.fold_in(jax.random.fold_in(rng, 6), axis_at), (blocks,), jnp.float32, smallest / len(shards), top_value / len(shards))
        factor_of = factor_of * jnp.repeat(jnp.exp(steps), dims[axis_at] // blocks).reshape((-1,) + (1,) * (len(dims) - 1 - axis_at))
    return factor_of


def bell_draw(rng, dims, deviation, reach, shards=(), held_as=jnp.bfloat16):
    entries = jax.random.normal(rng, dims, jnp.float32) * deviation
    if len(shards) > 0:
        entries = steps_of(rng, dims, shards, -0.22, 0.18) * entries
    return jnp.clip(entries, min=-reach, max=reach).astype(held_as)


def setup_inputs(seed: int = 0) -> dict:
    key_list = jax.random.split(jax.random.key(seed), 4)
    return {
        "mix_input": bell_draw(key_list[0], (SEQS, LENGTH, F), 1.0, 6.0, ((0, 4), (1, 8))),
        "gate_logits": bell_draw(key_list[1], (SEQS, LENGTH, D), 1.5, 8.0, ((0, 4), (1, 8))),
        "w_proj": bell_draw(key_list[2], (F, D), F ** -0.5, 0.1875, ((0, 4),)),
    }


def reference(mix_input, gate_logits, w_proj):
    def one_sequence(pair_args):
        signal, logits = pair_args
        grouped = signal.astype(jnp.float32).reshape(LENGTH, GROUPS, GROUP)
        spectrum = jnp.real(jnp.fft.fftn(grouped, axes=(0, 2), norm="ortho")).astype(jnp.float32)
        spectrum_bf = spectrum.reshape(LENGTH, GROUPS * GROUP).astype(jnp.bfloat16)
        projected = jnp.dot(spectrum_bf, w_proj, preferred_element_type=jnp.float32)
        return (jax.nn.sigmoid(logits.astype(jnp.float32)) * projected).astype(jnp.bfloat16)

    return lax.map(one_sequence, (mix_input, gate_logits))
```

```python
import functools
import math

import jax
import jax.numpy as jnp
import numpy as np
from jax import lax
from jax.experimental import pallas as pl
from jax.experimental.pallas import tpu as pltpu
from jax.sharding import PartitionSpec as P

MESH = pl.DeviceIdType.MESH
TAB_STEP = 32
OUT_CHUNK = 512

GROUP = 256
GROUPS = 4
POS_INNER = 128


highest = lax.Precision.HIGHEST


def tables(rows_in, cols_out, period):
    left_index = jnp.arange(rows_in, dtype=jnp.int32)[:, None]
    right_index = jnp.arange(cols_out, dtype=jnp.int32)[None, :]
    angles = (left_index * right_index % period).astype(jnp.float32) * (2.0 * math.pi / period)
    return (jnp.cos(angles), jnp.sin(angles))


def half_tables(group_size):
    index_row = jnp.arange(group_size, dtype=jnp.int32)
    frequency = jnp.where(index_row == 1, group_size // 2, index_row // 2)
    is_cosine = jnp.logical_or(index_row % 2 == 0, index_row == 1)
    channel = jnp.arange(group_size, dtype=jnp.int32)[:, None]
    angles = (channel * frequency[None, :] % group_size).astype(jnp.float32) * (
        2.0 * math.pi / group_size
    )
    return jnp.where(is_cosine[None, :], jnp.cos(angles), jnp.sin(angles))


def position_transform(values, inner_len):
    length, columns = values.shape
    outer_len = length // inner_len
    blocks = values.reshape(inner_len, outer_len, columns)
    cos_one, sin_one = tables(inner_len, inner_len, inner_len)
    first_re = jnp.einsum("pqc,pk->ckq", blocks, cos_one, precision=highest)
    first_im = -jnp.einsum("pqc,pk->ckq", blocks, sin_one, precision=highest)
    cos_twist, sin_twist = tables(inner_len, outer_len, length)
    second_re = first_re * cos_twist + first_im * sin_twist
    second_im = first_im * cos_twist - first_re * sin_twist
    cos_two, sin_two = tables(outer_len, outer_len, outer_len)
    whole_re = jnp.einsum("ckq,qj->cjk", second_re, cos_two, precision=highest) + jnp.einsum(
        "ckq,qj->cjk", second_im, sin_two, precision=highest
    )
    whole_im = jnp.einsum("ckq,qj->cjk", second_im, cos_two, precision=highest) - jnp.einsum(
        "ckq,qj->cjk", second_re, sin_two, precision=highest
    )
    return (whole_re.reshape(columns, length), whole_im.reshape(columns, length))


def on_device(mix_input, gate_logits, w_proj):
    tokens = mix_input[0]
    tok_count, features = tokens.shape
    row_count = lax.axis_size("row")
    length = tok_count * row_count
    norm_factor = 1.0 / math.sqrt(length * GROUP)
    grouped = tokens.astype(jnp.float32).reshape(tok_count, GROUPS, GROUP)
    packed = jnp.einsum("tgc,cm->tgm", grouped, half_tables(GROUP), precision=highest).reshape(
        tok_count, features
    )
    packed_cols = lax.all_to_all(packed, "row", split_axis=1, concat_axis=0, tiled=True)
    part_re, part_im = position_transform(packed_cols, POS_INNER)
    columns = part_re.shape[0]
    pair_re = part_re.reshape(columns // 2, 2, length)
    pair_im = part_im.reshape(columns // 2, 2, length)
    pair_index = lax.axis_index("row") * (columns // 2) + jnp.arange(columns // 2, dtype=jnp.int32)
    special = (pair_index % (GROUP // 2) == 0)[:, None]
    low_half = jnp.where(special, pair_re[:, 0], pair_re[:, 0] + pair_im[:, 1])
    high_half = jnp.where(special, pair_re[:, 1], pair_re[:, 0] - pair_im[:, 1])
    paired = (
        jnp.stack([low_half, high_half], axis=1).reshape(columns, length) * norm_factor
    ).astype(jnp.bfloat16)
    returned = lax.all_to_all(paired, "row", split_axis=1, concat_axis=0, tiled=True)
    pair_grid = returned.reshape(GROUPS, GROUP // 2, 2, tok_count)
    spectrum = jnp.concatenate(
        [pair_grid[:, :, 0], pair_grid[:, :1, 1], jnp.flip(pair_grid[:, 1:, 1], axis=1)], axis=1
    ).reshape(features, tok_count)
    projected = lax.dot_general(
        spectrum,
        lax.all_gather(w_proj, "col", axis=0, tiled=True),
        (((0,), (0,)), ((), ())),
        preferred_element_type=jnp.float32,
    )
    gate_open = jax.nn.sigmoid(gate_logits[0].astype(jnp.float32))
    return (gate_open * projected).astype(jnp.bfloat16)[None]


def channel_table(rows):
    half = GROUP // 2
    quarter = half // 2
    table = np.zeros((GROUP, GROUP))
    mixing = np.zeros((GROUP, GROUP))
    channel = np.arange(GROUP)
    for core in range(2):
        for i in range(quarter):
            m = quarter * core + i
            low, high = half * core + i, half * core + quarter + i
            angle = 2.0 * np.pi * (channel * m % GROUP) / GROUP
            table[:, low] = np.cos(angle)
            table[:, high] = np.sin(angle) if m else np.cos(np.pi * channel)
            mixing[low, m] = 1.0
            mixing[high, GROUP - m if m else half] = 1.0
    return table, mixing


def base_tables(length):
    position = np.arange(length)
    coarse = np.arange(length // 2 // TAB_STEP)[:, None] * TAB_STEP
    fine = np.arange(TAB_STEP)[:, None]
    step = 2.0 * np.pi / length
    coarse_angle = (coarse * position % length) * step
    fine_angle = (fine * position % length) * step
    return (
        np.stack([np.cos(coarse_angle), np.sin(coarse_angle)]).astype(np.float32),
        np.stack([np.cos(fine_angle), np.sin(fine_angle)]).astype(np.float32),
    )


def fused_kernel(
    rows,
    cols,
    norm_factor,
    x_hbm,
    gate_hbm,
    w_hbm,
    chan_hbm,
    mix_hbm,
    coarse_hbm,
    fine_hbm,
    out_hbm,
    xv,
    gv,
    wv,
    chan,
    mix,
    coarse,
    fine,
    send_x,
    recv_x,
    tab,
    rhs,
    send_y,
    spec,
    wall,
    sig,
    outv,
    load_sem,
    out_sem,
    sx,
    rx,
    sy,
    ry,
    sw,
    rw,
    sf,
    rf,
):
    f32, bf16 = jnp.float32, jnp.bfloat16
    row, col = lax.axis_index("row"), lax.axis_index("col")
    chip, core = row // 2, row % 2
    tok = xv.shape[0]
    width = recv_x.shape[1]
    length = recv_x.shape[0]
    half_len = length // 2
    half_rows = GROUP // 2

    loads = [
        pltpu.make_async_copy(src, dst, load_sem.at[i])
        for i, (src, dst) in enumerate(
            [
                (x_hbm, xv),
                (chan_hbm, chan),
                (w_hbm, wv),
                (mix_hbm, mix),
                (coarse_hbm, coarse),
                (fine_hbm, fine),
                (gate_hbm, gv),
            ]
        )
    ]
    for load in loads:
        load.start()

    barrier = pltpu.get_barrier_semaphore()
    for i in range(1, rows):
        pl.semaphore_signal(
            barrier, inc=1, device_id=(lax.rem(row + i, rows), col), device_id_type=MESH
        )
    for i in range(1, cols):
        pl.semaphore_signal(
            barrier, inc=1, device_id=(row, lax.rem(col + i, cols)), device_id_type=MESH
        )

    def x_copy(dest, source):
        return pltpu.make_async_remote_copy(
            src_ref=send_x.at[dest],
            dst_ref=recv_x.at[pl.ds(pl.multiple_of(source * tok, tok), tok), :],
            send_sem=sx.at[dest],
            recv_sem=rx.at[source],
            device_id=(dest, col),
            device_id_type=MESH,
        )

    def y_copy(dest, source):
        return pltpu.make_async_remote_copy(
            src_ref=send_y.at[dest],
            dst_ref=spec.at[:, pl.ds(pl.multiple_of(source * width, width), width)],
            send_sem=sy.at[dest],
            recv_sem=ry.at[source],
            device_id=(dest, col),
            device_id_type=MESH,
        )

    def w_part(owner, part):
        return wall.at[owner, pl.ds(pl.multiple_of(part * half_rows, half_rows), half_rows), :]

    def w_copy(dest, owner):
        return pltpu.make_async_remote_copy(
            src_ref=w_part(owner, core),
            dst_ref=w_part(owner, core),
            send_sem=sw.at[dest],
            recv_sem=rw.at[owner],
            device_id=(row, dest),
            device_id_type=MESH,
        )

    def f_copy(owner, part):
        return pltpu.make_async_remote_copy(
            src_ref=w_part(owner, part),
            dst_ref=w_part(owner, part),
            send_sem=sf.at[owner],
            recv_sem=rf.at[owner],
            device_id=(row + 1 - 2 * core, col),
            device_id_type=MESH,
        )

    loads[0].wait()
    loads[1].wait()
    pl.semaphore_wait(barrier, rows - 1 + cols - 1)

    for i in range(GROUPS):
        g = lax.rem(chip + GROUPS // 2 + i, GROUPS)
        packed = jnp.dot(
            xv[:, pl.ds(pl.multiple_of(g * GROUP, GROUP), GROUP)],
            chan[...],
            preferred_element_type=f32,
        ).astype(bf16)
        for part in range(2):
            dest = 2 * g + part
            block = packed[:, part * width : (part + 1) * width]

            @pl.when(dest != row)
            def _():
                send_x[dest] = block
                x_copy(dest, row).start()

            @pl.when(dest == row)
            def _():
                recv_x[pl.ds(pl.multiple_of(row * tok, tok), tok), :] = block

    loads[2].wait()
    loads[3].wait()
    wall[col] = jnp.dot(mix[...], wv[...], preferred_element_type=f32).astype(bf16)
    for i in range(1, cols):
        w_copy(lax.rem(col + i, cols), col).start()

    loads[4].wait()
    loads[5].wait()

    def make_rows(a, carry):
        at = pl.ds(pl.multiple_of(a * TAB_STEP, TAB_STEP), TAB_STEP)
        for n in range(0, length, 512):
            cc = coarse[0, pl.ds(a, 1), n : n + 512]
            cs = coarse[1, pl.ds(a, 1), n : n + 512]
            fc = fine[0, :, n : n + 512]
            fs = fine[1, :, n : n + 512]
            tab[at, n : n + 512] = (cc * fc - cs * fs).astype(bf16)
            tab[at, length + n : length + n + 512] = (cs * fc + cc * fs).astype(bf16)
        return carry

    lax.fori_loop(0, half_len // TAB_STEP, make_rows, 0)

    loads[6].wait()

    def open_gate(i, carry):
        at = pl.ds(pl.multiple_of(i * 16, 16), 16)
        sig[at, :] = jax.nn.sigmoid(gv[at, :].astype(f32))
        return carry

    lax.fori_loop(0, tok // 16, open_gate, 0)

    quarter = width // 2
    left = lax.broadcasted_iota(jnp.int32, (width, width), 0)
    right = lax.broadcasted_iota(jnp.int32, (width, width), 1)
    first = jnp.logical_and(core == 0, right % quarter == 0)
    cos_from = jnp.where(first, right, right % quarter)
    cos_pick = jnp.where(left == cos_from, 1.0, 0.0).astype(bf16)
    sign = jnp.where(first, 0.0, jnp.where(right < quarter, -1.0, 1.0))
    sin_pick = jnp.where(left == right % quarter + quarter, sign, 0.0).astype(bf16)
    odd = lax.broadcasted_iota(jnp.int32, (tok, width), 0) % 2
    flip = jnp.where(odd == 1, -1.0, 1.0)

    for i in range(rows):
        source = lax.rem(row + i, rows)

        @pl.when(source != row)
        def _():
            x_copy(source, source).wait_recv()

        at = pl.ds(pl.multiple_of(source * tok, tok), tok)
        block = recv_x[at, :]
        for base, pick in ((0, cos_pick), (length, sin_pick)):
            picked = jnp.dot(block, pick, preferred_element_type=f32)
            to = pl.ds(pl.multiple_of(base + source * tok, tok), tok)
            rhs[to, :width] = picked.astype(bf16)
            rhs[to, width:] = (picked * flip).astype(bf16)

    def position_block(e, carry):
        at = pl.ds(pl.multiple_of(e * tok, tok), tok)
        block = jnp.dot(tab[at, :], rhs[...], preferred_element_type=f32) * norm_factor
        block = block.astype(bf16)
        for part in range(2):
            dest = e + part * (rows // 2)
            piece = block[:, part * width : (part + 1) * width]

            @pl.when(dest != row)
            def _():
                send_y[dest] = piece
                y_copy(dest, row).start()

            @pl.when(dest == row)
            def _():
                spec[:, pl.ds(pl.multiple_of(row * width, width), width)] = piece

        return carry

    lax.fori_loop(0, rows // 2, position_block, 0)

    for i in range(1, cols):
        owner = lax.rem(col + i, cols)
        w_copy(owner, owner).wait_recv()
        f_copy(owner, core).start()

    for i in range(1, rows):
        source = lax.rem(row + i, rows)
        y_copy(source, source).wait_recv()
    for i in range(1, cols):
        owner = lax.rem(col + i, cols)
        f_copy(owner, 1 - core).wait_recv()

    chunks = outv.shape[1] // OUT_CHUNK

    def out_copy(j):
        at = pl.ds(pl.multiple_of(j * OUT_CHUNK, OUT_CHUNK), OUT_CHUNK)
        return pltpu.make_async_copy(outv.at[:, at], out_hbm.at[:, at], out_sem.at[j])

    def project(j, carry):
        at = pl.ds(pl.multiple_of(j * OUT_CHUNK, OUT_CHUNK), OUT_CHUNK)
        total = jnp.zeros((tok, OUT_CHUNK), f32)
        for g in range(GROUPS):
            total += jnp.dot(
                spec[:, g * GROUP : (g + 1) * GROUP], wall[g, :, at], preferred_element_type=f32
            )
        outv[:, at] = (sig[:, at] * total).astype(bf16)
        out_copy(j).start()
        return carry

    lax.fori_loop(0, chunks, project, 0)

    for i in range(1, rows):
        dest = lax.rem(row + i, rows)
        x_copy(dest, row).wait_send()
        y_copy(dest, row).wait_send()
    for i in range(1, cols):
        other = lax.rem(col + i, cols)
        w_copy(other, col).wait_send()
        f_copy(other, core).wait_send()
    for j in range(chunks):
        out_copy(j).wait()


def fused(rows, cols, mix_input, gate_logits, w_proj):
    bf16, f32 = jnp.bfloat16, jnp.float32
    tokens, gates = mix_input[0], gate_logits[0]
    tok, features = tokens.shape
    width_out = gates.shape[1]
    length = tok * rows
    width = features // rows
    table, mixing = channel_table(rows)
    coarse, fine = base_tables(length)
    dma = pltpu.SemaphoreType.DMA
    return pl.pallas_call(
        functools.partial(fused_kernel, rows, cols, 1.0 / math.sqrt(length * GROUP)),
        out_shape=jax.ShapeDtypeStruct((tok, width_out), bf16),
        in_specs=[pl.BlockSpec(memory_space=pl.ANY)] * 7,
        out_specs=pl.BlockSpec(memory_space=pl.ANY),
        scratch_shapes=[
            pltpu.VMEM(tokens.shape, bf16),
            pltpu.VMEM(gates.shape, bf16),
            pltpu.VMEM(w_proj.shape, bf16),
            pltpu.VMEM(table.shape, bf16),
            pltpu.VMEM(mixing.shape, bf16),
            pltpu.VMEM(coarse.shape, f32),
            pltpu.VMEM(fine.shape, f32),
            pltpu.VMEM((rows, tok, width), bf16),
            pltpu.VMEM((length, width), bf16),
            pltpu.VMEM((length // 2, 2 * length), bf16),
            pltpu.VMEM((2 * length, 2 * width), bf16),
            pltpu.VMEM((rows, tok, width), bf16),
            pltpu.VMEM((tok, features), bf16),
            pltpu.VMEM((cols, *w_proj.shape), bf16),
            pltpu.VMEM(gates.shape, f32),
            pltpu.VMEM(gates.shape, bf16),
            dma((7,)),
            dma((width_out // OUT_CHUNK,)),
            dma((rows,)),
            dma((rows,)),
            dma((rows,)),
            dma((rows,)),
            dma((cols,)),
            dma((cols,)),
            dma((cols,)),
            dma((cols,)),
        ],
        compiler_params=pltpu.CompilerParams(
            collective_id=0, has_side_effects=True, vmem_limit_bytes=48 * 1024 * 1024
        ),
    )(
        tokens,
        gates,
        w_proj,
        jnp.asarray(table, bf16),
        jnp.asarray(mixing, bf16),
        jnp.asarray(coarse),
        jnp.asarray(fine),
    )[None]


def fits(rows, cols, mix_input, gate_logits, w_proj):
    features = mix_input.shape[2]
    return (
        cols == GROUPS
        and rows == 2 * GROUPS
        and features == GROUPS * GROUP
        and w_proj.shape[0] == features
        and mix_input.shape[0] == cols
        and mix_input.shape[1] // rows % 128 == 0
        and mix_input.shape[1] <= 2048
        and gate_logits.shape[2] % OUT_CHUNK == 0
    )


def solution(mesh):
    rows, cols = mesh.shape["row"], mesh.shape["col"]
    in_specs = (P("col", "row", None), P("col", "row", None), P("col", None))
    out_specs = P("col", "row", None)

    def run(mix_input, gate_logits, w_proj):
        body = on_device
        if fits(rows, cols, mix_input, gate_logits, w_proj):
            body = functools.partial(fused, rows, cols)
        return jax.shard_map(
            body, mesh=mesh, in_specs=in_specs, out_specs=out_specs, check_vma=False
        )(mix_input, gate_logits, w_proj)

    return run
```

```python
import functools
import math

import jax
import jax.numpy as jnp
import numpy as np
from jax import lax
from jax.experimental import pallas as pl
from jax.experimental.pallas import tpu as pltpu
from jax.sharding import PartitionSpec as P

MESH = pl.DeviceIdType.MESH
TAB_STEP = 32
OUT_CHUNK = 512

GROUP = 256
GROUPS = 4
POS_INNER = 128


highest = lax.Precision.HIGHEST


def tables(rows_in, cols_out, period):
    left_index = jnp.arange(rows_in, dtype=jnp.int32)[:, None]
    right_index = jnp.arange(cols_out, dtype=jnp.int32)[None, :]
    angles = (left_index * right_index % period).astype(jnp.float32) * (2.0 * math.pi / period)
    return (jnp.cos(angles), jnp.sin(angles))


def half_tables(group_size):
    index_row = jnp.arange(group_size, dtype=jnp.int32)
    frequency = jnp.where(index_row == 1, group_size // 2, index_row // 2)
    is_cosine = jnp.logical_or(index_row % 2 == 0, index_row == 1)
    channel = jnp.arange(group_size, dtype=jnp.int32)[:, None]
    angles = (channel * frequency[None, :] % group_size).astype(jnp.float32) * (
        2.0 * math.pi / group_size
    )
    return jnp.where(is_cosine[None, :], jnp.cos(angles), jnp.sin(angles))


def position_transform(values, inner_len):
    length, columns = values.shape
    outer_len = length // inner_len
    blocks = values.reshape(inner_len, outer_len, columns)
    cos_one, sin_one = tables(inner_len, inner_len, inner_len)
    first_re = jnp.einsum("pqc,pk->ckq", blocks, cos_one, precision=highest)
    first_im = -jnp.einsum("pqc,pk->ckq", blocks, sin_one, precision=highest)
    cos_twist, sin_twist = tables(inner_len, outer_len, length)
    second_re = first_re * cos_twist + first_im * sin_twist
    second_im = first_im * cos_twist - first_re * sin_twist
    cos_two, sin_two = tables(outer_len, outer_len, outer_len)
    whole_re = jnp.einsum("ckq,qj->cjk", second_re, cos_two, precision=highest) + jnp.einsum(
        "ckq,qj->cjk", second_im, sin_two, precision=highest
    )
    whole_im = jnp.einsum("ckq,qj->cjk", second_im, cos_two, precision=highest) - jnp.einsum(
        "ckq,qj->cjk", second_re, sin_two, precision=highest
    )
    return (whole_re.reshape(columns, length), whole_im.reshape(columns, length))


def on_device(mix_input, gate_logits, w_proj):
    tokens = mix_input[0]
    tok_count, features = tokens.shape
    row_count = lax.axis_size("row")
    length = tok_count * row_count
    norm_factor = 1.0 / math.sqrt(length * GROUP)
    grouped = tokens.astype(jnp.float32).reshape(tok_count, GROUPS, GROUP)
    packed = jnp.einsum("tgc,cm->tgm", grouped, half_tables(GROUP), precision=highest).reshape(
        tok_count, features
    )
    packed_cols = lax.all_to_all(packed, "row", split_axis=1, concat_axis=0, tiled=True)
    part_re, part_im = position_transform(packed_cols, POS_INNER)
    columns = part_re.shape[0]
    pair_re = part_re.reshape(columns // 2, 2, length)
    pair_im = part_im.reshape(columns // 2, 2, length)
    pair_index = lax.axis_index("row") * (columns // 2) + jnp.arange(columns // 2, dtype=jnp.int32)
    special = (pair_index % (GROUP // 2) == 0)[:, None]
    low_half = jnp.where(special, pair_re[:, 0], pair_re[:, 0] + pair_im[:, 1])
    high_half = jnp.where(special, pair_re[:, 1], pair_re[:, 0] - pair_im[:, 1])
    paired = (
        jnp.stack([low_half, high_half], axis=1).reshape(columns, length) * norm_factor
    ).astype(jnp.bfloat16)
    returned = lax.all_to_all(paired, "row", split_axis=1, concat_axis=0, tiled=True)
    pair_grid = returned.reshape(GROUPS, GROUP // 2, 2, tok_count)
    spectrum = jnp.concatenate(
        [pair_grid[:, :, 0], pair_grid[:, :1, 1], jnp.flip(pair_grid[:, 1:, 1], axis=1)], axis=1
    ).reshape(features, tok_count)
    projected = lax.dot_general(
        spectrum,
        lax.all_gather(w_proj, "col", axis=0, tiled=True),
        (((0,), (0,)), ((), ())),
        preferred_element_type=jnp.float32,
    )
    gate_open = jax.nn.sigmoid(gate_logits[0].astype(jnp.float32))
    return (gate_open * projected).astype(jnp.bfloat16)[None]


def channel_table():
    half, part = GROUP // 2, GROUP // 8
    table = np.zeros((2, GROUP, GROUP))
    mixing = np.zeros((GROUP, GROUP))
    channel = np.arange(GROUP)
    for stage in range(2):
        for core in range(2):
            for i in range(part):
                m = 2 * part * core + part * stage + i
                angle = 2.0 * np.pi * (channel * m % GROUP) / GROUP
                pair = (np.cos(angle), np.sin(angle) if m else np.cos(np.pi * channel))
                for which in range(2):
                    at = half * stage + part * which + i
                    table[0, :, at + 2 * part * core] = pair[which]
                    table[1, :, at + 2 * part * (1 - core)] = pair[which]
                low = half * stage + 2 * part * core + i
                mixing[low, m] = 1.0
                mixing[low + part, GROUP - m if m else half] = 1.0
    return table, mixing


def base_tables(length):
    position = np.arange(length)
    coarse = np.arange(length // 2 // TAB_STEP)[:, None] * TAB_STEP
    fine = np.arange(TAB_STEP)[:, None]
    step = 2.0 * np.pi / length
    coarse_angle = (coarse * position % length) * step
    fine_angle = (fine * position % length) * step
    return (
        np.stack([np.cos(coarse_angle), np.sin(coarse_angle)]).astype(np.float32),
        np.stack([np.cos(fine_angle), np.sin(fine_angle)]).astype(np.float32),
    )


def fused_kernel(
    rows,
    cols,
    norm_factor,
    x_hbm,
    gate_hbm,
    w_hbm,
    chan_hbm,
    mix_hbm,
    coarse_hbm,
    fine_hbm,
    out_hbm,
    xv,
    gv,
    wv,
    chan,
    mix,
    coarse,
    fine,
    send_x,
    recv_x,
    tab,
    rhs,
    send_y,
    recv_y,
    spec,
    wall,
    sig,
    acc,
    outv,
    load_sem,
    out_sem,
    sx,
    rx,
    sy,
    ry,
    sw,
    rw,
    sf,
    rf,
):
    f32, bf16 = jnp.float32, jnp.bfloat16
    row, col = lax.axis_index("row"), lax.axis_index("col")
    chip, core = row // 2, row % 2
    tok = xv.shape[0]
    half_tok = tok // 2
    lanes = recv_x.shape[3]
    length = tok * rows
    half_len = length // 2
    upper = row // (rows // 2)

    loads = [
        pltpu.make_async_copy(src, dst, load_sem.at[i])
        for i, (src, dst) in enumerate(
            [
                (x_hbm, xv),
                (chan_hbm, chan),
                (w_hbm, wv),
                (mix_hbm, mix),
                (coarse_hbm, coarse),
                (fine_hbm, fine),
                (gate_hbm, gv),
            ]
        )
    ]
    for load in loads:
        load.start()

    barrier = pltpu.get_barrier_semaphore()
    for i in range(1, rows):
        pl.semaphore_signal(
            barrier, inc=1, device_id=(lax.rem(row + i, rows), col), device_id_type=MESH
        )
    for i in range(1, cols):
        pl.semaphore_signal(
            barrier, inc=1, device_id=(row, lax.rem(col + i, cols)), device_id_type=MESH
        )

    def x_copy(h, dest, source):
        return pltpu.make_async_remote_copy(
            src_ref=send_x.at[h, dest],
            dst_ref=recv_x.at[h, source],
            send_sem=sx.at[h, dest],
            recv_sem=rx.at[h, source],
            device_id=(dest, col),
            device_id_type=MESH,
        )

    def y_copy(h, dest, source):
        return pltpu.make_async_remote_copy(
            src_ref=send_y.at[h, dest],
            dst_ref=recv_y.at[h, source],
            send_sem=sy.at[h, dest],
            recv_sem=ry.at[h, source],
            device_id=(dest, col),
            device_id_type=MESH,
        )

    def w_part(owner, part):
        return wall.at[part, pl.ds(pl.multiple_of(owner * lanes, lanes), lanes), :]

    def w_piece(owner, piece):
        size = lanes // 2
        start = pl.multiple_of(owner * lanes + piece * size, size)
        return wall.at[core, pl.ds(start, size), :]

    def w_copy(dest, owner, slot, piece):
        return pltpu.make_async_remote_copy(
            src_ref=w_piece(owner, piece),
            dst_ref=w_piece(owner, piece),
            send_sem=sw.at[slot, piece],
            recv_sem=rw.at[owner, piece],
            device_id=(row, dest),
            device_id_type=MESH,
        )

    def f_copy(owner, part):
        return pltpu.make_async_remote_copy(
            src_ref=w_part(owner, part),
            dst_ref=w_part(owner, part),
            send_sem=sf.at[owner],
            recv_sem=rf.at[owner],
            device_id=(row + 1 - 2 * core, col),
            device_id_type=MESH,
        )

    col_x = col + 1 - 2 * (col % 2)
    col_y = lax.rem(col + 2, cols)
    col_far = lax.rem(col_x + 2, cols)
    relay_from = jnp.where(core == 0, col_x, col_y)
    relay_to = jnp.where(core == 0, col_y, col_x)
    low_lanes = lax.broadcasted_iota(jnp.int32, (half_tok, lanes), 1) < lanes // 2

    def channel_stage(h, carry):
        to = pl.ds(pl.multiple_of(h * lanes, lanes), lanes)
        for g in range(GROUPS):
            at = slice(g * GROUP, (g + 1) * GROUP)
            top = jnp.dot(xv[:half_tok, at], chan[0, :, to], preferred_element_type=f32)
            low = jnp.dot(xv[half_tok:, at], chan[1, :, to], preferred_element_type=f32)
            for part in range(2):
                pick = low_lanes if part == 0 else jnp.logical_not(low_lanes)
                send_x[h, 2 * g + part] = jnp.where(pick, top, low).astype(bf16)
        recv_x[h, row] = send_x[h, row]
        return carry

    def send_stage(h):
        for i in range(rows):
            dest = lax.rem(2 * chip + rows // 2 + i, rows)

            @pl.when(dest != row)
            def _():
                x_copy(h, dest, row).start()

    loads[0].wait()
    loads[1].wait()
    channel_stage(0, 0)
    loads[2].wait()
    loads[3].wait()
    mixed_w = jnp.dot(mix[...], wv[...], preferred_element_type=f32).astype(bf16)
    for h in range(2):
        w_part(col, h)[...] = mixed_w[h * lanes : (h + 1) * lanes]
    pl.semaphore_wait(barrier, rows - 1 + cols - 1)
    send_stage(0)
    for piece in range(2):
        w_copy(col_x, col, 0, piece).start()
        w_copy(col_y, col, 1, piece).start()
    channel_stage(1, 0)
    send_stage(1)

    loads[4].wait()
    loads[5].wait()

    def make_rows(a, carry):
        at = pl.ds(pl.multiple_of(a * TAB_STEP, TAB_STEP), TAB_STEP)
        for n in range(0, length, 512):
            cc = coarse[0, pl.ds(a, 1), n : n + 512]
            cs = coarse[1, pl.ds(a, 1), n : n + 512]
            fc = fine[0, :, n : n + 512]
            fs = fine[1, :, n : n + 512]
            tab[at, n : n + 512] = (cc * fc - cs * fs).astype(bf16)
            tab[at, length + n : length + n + 512] = (cs * fc + cc * fs).astype(bf16)
        return carry

    lax.fori_loop(0, half_len // TAB_STEP, make_rows, 0)

    quarter = lanes // 4
    left = lax.broadcasted_iota(jnp.int32, (lanes, lanes), 0)
    right = lax.broadcasted_iota(jnp.int32, (lanes, lanes), 1)
    slot = right % (2 * quarter)
    odd = lax.broadcasted_iota(jnp.int32, (half_tok, lanes), 0) % 2 == 1
    flip = jnp.where(jnp.logical_and(odd, jnp.logical_not(low_lanes)), -1.0, 1.0)

    def position_stage(h):
        first = jnp.logical_and(core == 0, slot % quarter == 0)
        if h > 0:
            first = jnp.logical_and(first, slot < 0)
        cos_from = jnp.where(first, slot, slot % quarter)
        sin_from = slot % quarter + quarter
        sign = jnp.where(first, 0.0, jnp.where(slot < quarter, -1.0, 1.0))
        picks = []
        for part in range(2):
            offset = 2 * quarter * jnp.where(core == part, 0, 1)
            picks.append(
                (
                    jnp.where(left == cos_from + offset, 1.0, 0.0).astype(bf16),
                    jnp.where(left == sin_from + offset, sign, 0.0).astype(bf16),
                )
            )

        for i in range(rows):
            source = lax.rem(row + i, rows)

            @pl.when(source != row)
            def _():
                x_copy(h, source, source).wait_recv()

            block = recv_x[h, source]
            for part in range(2):
                for which in range(2):
                    picked = jnp.dot(block, picks[part][which], preferred_element_type=f32)
                    start = which * length + source * tok + part * half_tok
                    to = pl.ds(pl.multiple_of(start, half_tok), half_tok)
                    rhs[h, to, :] = (picked * flip).astype(bf16)

        def position_block(e, carry):
            at = pl.ds(pl.multiple_of(e * tok, tok), tok)
            block = jnp.dot(tab[at, :], rhs[h], preferred_element_type=f32) * norm_factor
            top = block[:half_tok]
            low = pltpu.roll(block[half_tok:], lanes // 2, 1)
            for part in range(2):
                dest = e + part * (rows // 2)
                pick = low_lanes if part == 0 else jnp.logical_not(low_lanes)
                piece = jnp.where(pick, top, low).astype(bf16)

                @pl.when(dest != row)
                def _():
                    send_y[h, dest] = piece
                    y_copy(h, dest, row).start()

                @pl.when(dest == row)
                def _():
                    recv_y[h, row] = piece

            return carry

        lax.fori_loop(0, rows // 2, position_block, 0)

    def collect(h):
        for i in range(1, rows):
            source = lax.rem(row + i, rows)
            y_copy(h, source, source).wait_recv()
        for g in range(GROUPS):
            one = recv_y[h, 2 * g].astype(f32)
            two = recv_y[h, 2 * g + 1].astype(f32)
            kept = jnp.where(low_lanes, one, pltpu.roll(two, lanes // 2, 1)).astype(bf16)
            moved = jnp.where(low_lanes, pltpu.roll(one, lanes // 2, 1), two).astype(bf16)
            to = slice(g * lanes, (g + 1) * lanes)
            spec[h, pl.ds(pl.multiple_of(upper * half_tok, half_tok), half_tok), to] = kept
            spec[h, pl.ds(pl.multiple_of((1 - upper) * half_tok, half_tok), half_tok), to] = moved

    w_copy(relay_from, relay_from, 0, 0).wait_recv()
    w_copy(relay_to, relay_from, 2, 0).start()
    position_stage(0)
    w_copy(relay_from, relay_from, 0, 1).wait_recv()
    w_copy(relay_to, relay_from, 2, 1).start()
    for piece in range(2):
        w_copy(relay_to, relay_to, 1, piece).wait_recv()
    f_copy(col_x, core).start()
    f_copy(col_y, core).start()

    position_stage(1)

    loads[6].wait()

    def open_gate(i, carry):
        at = pl.ds(pl.multiple_of(i * 16, 16), 16)
        sig[at, :] = jax.nn.sigmoid(gv[at, :].astype(f32))
        return carry

    lax.fori_loop(0, tok // 16, open_gate, 0)

    for piece in range(2):
        w_copy(col_far, col_far, 2, piece).wait_recv()
    f_copy(col_far, core).start()

    chunks = outv.shape[1] // OUT_CHUNK

    def chunk_at(j):
        return pl.ds(pl.multiple_of(j * OUT_CHUNK, OUT_CHUNK), OUT_CHUNK)

    def out_copy(j):
        return pltpu.make_async_copy(
            outv.at[:, chunk_at(j)], out_hbm.at[:, chunk_at(j)], out_sem.at[j]
        )

    collect(0)
    for owner in (col_x, col_y, col_far):
        f_copy(owner, 1 - core).wait_recv()

    def project_first(j, carry):
        at = chunk_at(j)
        acc[:, at] = jnp.dot(spec[0], wall[0, :, at], preferred_element_type=f32)
        return carry

    lax.fori_loop(0, chunks, project_first, 0)
    collect(1)

    def project(j, carry):
        at = chunk_at(j)
        total = acc[:, at] + jnp.dot(spec[1], wall[1, :, at], preferred_element_type=f32)
        outv[:, at] = (sig[:, at] * total).astype(bf16)
        out_copy(j).start()
        return carry

    lax.fori_loop(0, chunks, project, 0)

    for i in range(1, rows):
        dest = lax.rem(row + i, rows)
        for h in range(2):
            x_copy(h, dest, row).wait_send()
            y_copy(h, dest, row).wait_send()
    for piece in range(2):
        w_copy(col_x, col, 0, piece).wait_send()
        w_copy(col_y, col, 1, piece).wait_send()
        w_copy(relay_to, relay_from, 2, piece).wait_send()
    for owner in (col_x, col_y, col_far):
        f_copy(owner, core).wait_send()
    for j in range(chunks):
        out_copy(j).wait()


def fused(rows, cols, mix_input, gate_logits, w_proj):
    bf16, f32 = jnp.bfloat16, jnp.float32
    tokens, gates = mix_input[0], gate_logits[0]
    tok, features = tokens.shape
    width_out = gates.shape[1]
    length = tok * rows
    width = features // rows
    table, mixing = channel_table()
    coarse, fine = base_tables(length)
    dma = pltpu.SemaphoreType.DMA
    return pl.pallas_call(
        functools.partial(fused_kernel, rows, cols, 1.0 / math.sqrt(length * GROUP)),
        out_shape=jax.ShapeDtypeStruct((tok, width_out), bf16),
        in_specs=[pl.BlockSpec(memory_space=pl.ANY)] * 7,
        out_specs=pl.BlockSpec(memory_space=pl.ANY),
        scratch_shapes=[
            pltpu.VMEM(tokens.shape, bf16),
            pltpu.VMEM(gates.shape, bf16),
            pltpu.VMEM(w_proj.shape, bf16),
            pltpu.VMEM(table.shape, bf16),
            pltpu.VMEM(mixing.shape, bf16),
            pltpu.VMEM(coarse.shape, f32),
            pltpu.VMEM(fine.shape, f32),
            pltpu.VMEM((2, rows, tok // 2, width), bf16),
            pltpu.VMEM((2, rows, tok // 2, width), bf16),
            pltpu.VMEM((length // 2, 2 * length), bf16),
            pltpu.VMEM((2, 2 * length, width), bf16),
            pltpu.VMEM((2, rows, tok // 2, width), bf16),
            pltpu.VMEM((2, rows, tok // 2, width), bf16),
            pltpu.VMEM((2, tok, features // 2), bf16),
            pltpu.VMEM((2, features // 2, width_out), bf16),
            pltpu.VMEM(gates.shape, f32),
            pltpu.VMEM(gates.shape, f32),
            pltpu.VMEM(gates.shape, bf16),
            dma((7,)),
            dma((width_out // OUT_CHUNK,)),
            dma((2, rows)),
            dma((2, rows)),
            dma((2, rows)),
            dma((2, rows)),
            dma((3, 2)),
            dma((cols, 2)),
            dma((cols,)),
            dma((cols,)),
        ],
        compiler_params=pltpu.CompilerParams(
            collective_id=0, has_side_effects=True, vmem_limit_bytes=67043328
        ),
    )(
        tokens,
        gates,
        w_proj,
        jnp.asarray(table, bf16),
        jnp.asarray(mixing, bf16),
        jnp.asarray(coarse),
        jnp.asarray(fine),
    )[None]


def fits(rows, cols, mix_input, gate_logits, w_proj):
    features = mix_input.shape[2]
    return (
        cols == GROUPS
        and rows == 2 * GROUPS
        and features == GROUPS * GROUP
        and w_proj.shape[0] == features
        and features // rows == 128
        and mix_input.shape[0] == cols
        and mix_input.shape[1] // rows % 256 == 0
        and mix_input.shape[1] <= 2048
        and gate_logits.shape[2] % OUT_CHUNK == 0
    )


def solution(mesh):
    rows, cols = mesh.shape["row"], mesh.shape["col"]
    in_specs = (P("col", "row", None), P("col", "row", None), P("col", None))
    out_specs = P("col", "row", None)

    def run(mix_input, gate_logits, w_proj):
        body = on_device
        if fits(rows, cols, mix_input, gate_logits, w_proj):
            body = functools.partial(fused, rows, cols)
        return jax.shard_map(
            body, mesh=mesh, in_specs=in_specs, out_specs=out_specs, check_vma=False
        )(mix_input, gate_logits, w_proj)

    return run
```
